512 devices in a mesh: sp: 32 (over z, x), dp: 16 (over y, core).
Axes of the slice: x: 4, y: 8, z: 8, core: 2. Of those that a mesh axis runs over, the one named last changes fastest.
Arguments:
- normed_input: bfloat16 [10240, 2048], P('sp'), may hold values from -6 to 6
- out_grad: bfloat16 [10240, 2048], P('sp'), may hold values from -6 to 6
- value_weight: bfloat16 [2048, 1024], P(None, 'dp'), may hold values from -0.125 to 0.125
- gate_weight: bfloat16 [2048, 1024], P(None, 'dp'), may hold values from -0.125 to 0.125
- down_weight: bfloat16 [1024, 2048], P('dp'), may hold values from -0.1875 to 0.1875
- conv_kernel: float32 [31, 1024], P(None, 'dp'), may hold values from -5 to 5
- conv_bias: float32 [1024], P('dp'), may hold values from -3 to 3
- norm_gain: float32 [1024], P('dp'), may hold values from 0.1 to 1.9
- norm_shift: float32 [1024], P('dp'), may hold values from -3 to 3
Outputs:
- input_grad: bfloat16 [10240, 2048], P('sp')
- value_grad: float32 [2048, 1024], P('sp', 'dp')
- gate_grad: float32 [2048, 1024], P('sp', 'dp')
- down_grad: float32 [1024, 2048], P('dp', 'sp')
- kernel_grad: float32 [31, 1024], P(None, 'dp')
- bias_grad: float32 [1024], P('dp')
- gain_grad: float32 [1024], P('dp')
- shift_grad: float32 [1024], P('dp')
The draws below stay inside these ranges and needn't reach their ends.
All inputs are finite; a program needn't handle non-finite values.
Results may differ from the reference program's by a relative error of at most 0.006.
Values may be sent and summed in bfloat16 or wider, within the bound.
A program may use at most 64 MiB of HBM per device.

```python
import math
import jax
import jax.numpy as jnp
from jax import lax

D = 2048
C = 1024
KW = 31
TOKENS = 10240


def draw_conv_kernel(key, part):
    first, second = jax.random.split(jax.random.fold_in(key, 11))
    place = jnp.arange(C, dtype=jnp.float32) / C
    jitter = jax.random.uniform(first, (C,), jnp.float32, -0.25, 0.25)
    scale = jnp.exp(jnp.log(0.5) + jnp.log(10.0) * place + jitter)
    base = jnp.clip(jax.random.normal(second, (KW, C), jnp.float32), -4.0, 4.0)
    return base * scale[None, :] / math.sqrt(KW)


def draw_conv_bias(key, part):
    noise_key = jax.random.fold_in(key, 23)
    place = jnp.arange(C, dtype=jnp.float32) / C
    noise = jnp.clip(jax.random.normal(noise_key, (C,), jnp.float32), -4.0, 4.0)
    return -0.8 + 2.0 * place + 0.4 * noise


def strengthened(array, key, source, target, blocks, factor):
    def block_of(dim):
        return (jnp.arange(array.shape[dim]) // (array.shape[dim] // blocks)).reshape((-1,) + (1,) * (array.ndim - 1 - dim))

    one_side = jax.random.permutation(key, blocks)[block_of(target)]
    second = (block_of(target) + blocks // 2) % blocks
    return jnp.where((block_of(source) == one_side) | (block_of(source) == second), factor * array, array)


def steps_of(key, shape, shards, least, high):
    gain, own = 1.0, jax.random.fold_in(key, 6)
    for axis_at, blocks in shards:
        draws = jnp.exp(jax.random.uniform(jax.random.fold_in(own, axis_at), (blocks,), jnp.float32, least / len(shards), high / len(shards)))
        gain = gain * jnp.repeat(draws, shape[axis_at] // blocks).reshape([-1 if axis == axis_at else 1 for axis in range(len(shape))])
    return gain


def bell_draw(rng, shape, scale, bound, cuts=(), kind=jnp.bfloat16):
    values = scale * jax.random.normal(rng, shape, jnp.float32)
    if cuts:
        values = values * steps_of(rng, shape, cuts, -0.22, 0.18)
    return jnp.clip(values, -bound, bound).astype(kind)


def heavy_noise(own_key, extent, scale, most, pieces, heavy, kind=jnp.bfloat16):
    values = scale * jax.random.normal(own_key, extent, jnp.float32)
    if pieces:
        values = values * steps_of(own_key, extent, pieces, -0.22, 0.18)
    return jnp.clip(strengthened(values, jax.random.fold_in(own_key, 3), *heavy), -most, most).astype(kind)


def setup_inputs(seed: int = 0) -> dict:
    keys = jax.random.split(jax.random.key(seed), 10)
    normed_input = heavy_noise(keys[0], (TOKENS, D), 1.0, 6.0, ((0, 32),), (0, 1, 32, 2.75))
    out_grad = heavy_noise(keys[1], (TOKENS, D), 1.0, 6.0, ((0, 32),), (0, 1, 32, 2.75))
    value_weight = bell_draw(keys[2], (D, C), D ** -0.5, 0.125, ((1, 16),))
    gate_weight = bell_draw(keys[3], (D, C), D ** -0.5, 0.125, ((1, 16),))
    down_weight = bell_draw(keys[4], (C, D), C ** -0.5, 0.1875, ((0, 16),))
    conv_kernel = draw_conv_kernel(jax.random.fold_in(keys[9], 71), 0)
    conv_bias = draw_conv_bias(jax.random.fold_in(keys[9], 71), 0)
    norm_gain = jnp.clip(1.0 + 0.18 * jax.random.normal(keys[7], (C,), jnp.float32), 0.1, 1.9)
    norm_shift = bell_draw(keys[8], (C,), 0.5, 3.0, ((0, 16),), jnp.float32)
    return {"normed_input": normed_input, "out_grad": out_grad, "value_weight": value_weight, "gate_weight": gate_weight, "down_weight": down_weight, "conv_kernel": conv_kernel, "conv_bias": conv_bias, "norm_gain": norm_gain, "norm_shift": norm_shift}


EPS = 1e-05

def reference(normed_input, out_grad, value_weight, gate_weight, down_weight, conv_kernel, conv_bias, norm_gain, norm_shift):
    reach = KW // 2
    ratio = 1.0 / math.sqrt(TOKENS)
    value_b = jnp.dot(normed_input, value_weight, preferred_element_type=jnp.float32).astype(jnp.bfloat16)
    gate_b = jnp.dot(normed_input, gate_weight, preferred_element_type=jnp.float32).astype(jnp.bfloat16)
    value = lax.optimization_barrier(value_b).astype(jnp.float32)
    gate = lax.optimization_barrier(gate_b).astype(jnp.float32)
    opening = jax.nn.sigmoid(gate)
    glu = value * opening
    padded = jnp.pad(glu, ((reach, reach), (0, 0)))
    mixed = jnp.zeros_like(glu) + conv_bias[None, :]
    for tap in range(KW):
        mixed = mixed + conv_kernel[tap][None, :] * padded[tap:tap + TOKENS]
    mean = lax.optimization_barrier(jnp.mean(mixed, axis=1, keepdims=True))
    spread = lax.optimization_barrier(jnp.mean((mixed - mean) * (mixed - mean), axis=1, keepdims=True))
    inv_std = lax.rsqrt(spread + EPS)
    centred = (mixed - mean) * inv_std
    normed = centred * norm_gain[None, :] + norm_shift[None, :]
    sig = jax.nn.sigmoid(normed)
    activated = (normed * sig).astype(jnp.bfloat16)
    d_act = jnp.dot(out_grad, down_weight.T, preferred_element_type=jnp.float32)
    d_normed = d_act * sig * (1.0 + normed * (1.0 - sig))
    d_centred = d_normed * norm_gain[None, :]
    first = lax.optimization_barrier(jnp.mean(d_centred, axis=1, keepdims=True))
    second = lax.optimization_barrier(jnp.mean(d_centred * centred, axis=1, keepdims=True))
    d_mixed = inv_std * (d_centred - first - centred * second)
    d_padded = jnp.pad(d_mixed, ((reach, reach), (0, 0)))
    d_glu = jnp.zeros_like(d_mixed)
    for tap in range(KW):
        d_glu = d_glu + conv_kernel[tap][None, :] * d_padded[2 * reach - tap:2 * reach - tap + TOKENS]
    kernel_grad = jnp.stack([lax.optimization_barrier(jnp.sum(d_mixed * padded[tap:tap + TOKENS], axis=0)) for tap in range(KW)]) * ratio
    bias_grad = lax.optimization_barrier(jnp.sum(d_mixed, axis=0)) * ratio
    gain_grad = lax.optimization_barrier(jnp.sum(d_normed * centred, axis=0)) * ratio
    shift_grad = lax.optimization_barrier(jnp.sum(d_normed, axis=0)) * ratio
    d_value = (d_glu * opening).astype(jnp.bfloat16)
    d_gate = (d_glu * value * opening * (1.0 - opening)).astype(jnp.bfloat16)
    value_grad = jnp.dot(normed_input.T, d_value, preferred_element_type=jnp.float32) * ratio
    gate_grad = jnp.dot(normed_input.T, d_gate, preferred_element_type=jnp.float32) * ratio
    down_grad = jnp.dot(activated.T, out_grad, preferred_element_type=jnp.float32) * ratio
    input_grad = (jnp.dot(d_value, value_weight.T, preferred_element_type=jnp.float32) + jnp.dot(d_gate, gate_weight.T, preferred_element_type=jnp.float32)).astype(jnp.bfloat16)
    return (input_grad, value_grad, gate_grad, down_grad, kernel_grad, bias_grad, gain_grad, shift_grad)
```

```python
import functools
import math

import jax
import jax.numpy as jnp
from jax import lax
from jax.experimental import pallas as pl
from jax.experimental.pallas import tpu as pltpu
from jax.sharding import PartitionSpec as P

EPS = 1e-05
MESH = pl.DeviceIdType.MESH
X = 4
F32 = jnp.float32
BF16 = jnp.bfloat16
NT = (((1,), (1,)), ((), ()))
NN = (((1,), (0,)), ((), ()))
TN = (((0,), (0,)), ((), ()))
CHUNKS = 4


def dot(a, b, dims):
    return lax.dot_general(a, b, dims, preferred_element_type=F32)


def exact_dot(a, b, dims):
    return lax.dot_general(
        a, b, dims, precision=lax.Precision.HIGHEST, preferred_element_type=F32
    )


def aligned(index, size):
    return pl.ds(pl.multiple_of(index * size, size), size)


def repeat(low, high, body):
    def step(i, carry):
        body(i)
        return carry

    lax.fori_loop(low, high, step, 0)


class RingGather:
    def __init__(self, buf, rows, y, c, count, ring_send, ring_recv, pair_send, pair_recv):
        self.buf, self.rows, self.y, self.c, self.count = buf, rows, y, c, count
        self.ring_send, self.ring_recv = ring_send, ring_recv
        self.pair_send, self.pair_recv = pair_send, pair_recv
        self.half = count // 2

    def copy(self, owner, core, k, target, send, recv):
        ref = self.buf.at[aligned(k, self.rows), aligned(owner * 2 + core, 128)]
        return pltpu.make_async_remote_copy(
            ref, ref, send, recv, device_id={"dp": target}, device_id_type=MESH
        )

    def owner(self, way, h):
        step = -1 - h if way == 0 else 1 + h
        return lax.rem(self.y + step + self.count, self.count)

    def place(self, way, h):
        return self.count - 1 - h if way == 0 else 1 + h

    def takes(self, way, h, part):
        return h < self.half - 1 or (h == self.half - 1 and way == part)

    def ring(self, way, h, k, owner):
        step = 1 if way == 0 else self.count - 1
        target = lax.rem(self.y + step, self.count) * 2 + self.c
        return self.copy(
            owner, self.c, k, target, self.ring_send.at[way, h, k], self.ring_recv.at[way, h, k]
        )

    def pair(self, place, k, owner, core):
        return self.copy(
            owner,
            core,
            k,
            self.y * 2 + 1 - self.c,
            self.pair_send.at[place, k],
            self.pair_recv.at[place, k],
        )

    def start(self, k):
        for way in (0, 1):
            self.ring(way, 0, k, self.y).start()
        self.pair(0, k, self.y, self.c).start()

    def arrive(self, h, k, part):
        for way in (0, 1):
            if self.takes(way, h, part):
                owner = self.owner(way, h)
                self.ring(way, h, k, owner).wait_recv()
                if self.takes(way, h + 1, part):
                    self.ring(way, h + 1, k, owner).start()
                self.pair(self.place(way, h), k, owner, self.c).start()

    def hop(self, h):
        cut = CHUNKS // 2
        repeat(0, cut, lambda k: self.arrive(h, k, 0))
        repeat(cut, CHUNKS, lambda k: self.arrive(h, k, 1))

    def wait_pairs(self, k):
        for place in range(self.count):
            owner = lax.rem(self.y + place, self.count)
            self.pair(place, k, owner, 1 - self.c).wait_recv()

    def drain(self):
        cut = CHUNKS // 2
        for part, low, high in ((0, 0, cut), (1, cut, CHUNKS)):

            def body(k, part=part):
                for way in (0, 1):
                    for h in range(self.half):
                        if self.takes(way, h, part):
                            self.ring(way, h, k, self.y).wait_send()
                for place in range(self.count):
                    self.pair(place, k, self.y, self.c).wait_send()

            repeat(low, high, body)


def kernel(
    n_sp,
    n_dp,
    x_hbm,
    og_hbm,
    wv_hbm,
    wg_hbm,
    dw_hbm,
    ck_ref,
    cb_ref,
    ng_ref,
    ns_ref,
    ig_hbm,
    vg_out,
    dg_out,
    kg_out,
    x_ref,
    og_ref,
    wv_ref,
    wg_ref,
    dw_ref,
    w_ref,
    wall_ref,
    vg_ref,
    glu_ref,
    open_ref,
    dact_ref,
    mix_ref,
    cen_ref,
    inv_ref,
    dn_ref,
    dc_ref,
    act_ref,
    dm_ref,
    dvg_ref,
    g_ref,
    out_ref,
    stat_ref,
    pd_ref,
    pv_ref,
    rd_ref,
    rv_ref,
    s_ref,
    own_ref,
    rz_ref,
    kx_ref,
    kz_ref,
    load_sem,
    halo_send,
    halo_recv,
    wsend,
    wrecv,
    ssend,
    srecv,
    ring_send,
    ring_recv,
    pair_send,
    pair_recv,
    xsend,
    xrecv,
    zsend,
    zrecv,
    store_sem,
):
    T, D = x_ref.shape
    CL = cb_ref.shape[-1]
    KW = ck_ref.shape[0]
    C = CL * n_dp
    Z = n_sp // X
    Y = n_dp // 2
    PR = D // n_sp
    ratio = 1.0 / math.sqrt(T * n_sp)
    sp, dp = lax.axis_index("sp"), lax.axis_index("dp")
    z, x = sp // X, lax.rem(sp, X)
    y, c = dp // 2, lax.rem(dp, 2)

    loads = [
        pltpu.make_async_copy(a, b, load_sem.at[i])
        for i, (a, b) in enumerate(
            (
                (wv_hbm, wv_ref),
                (wg_hbm, wg_ref),
                (x_hbm, x_ref),
                (og_hbm, og_ref),
                (dw_hbm, dw_ref),
            )
        )
    ]
    for load in loads:
        load.start()

    def peer_dp(off):
        return lax.rem(dp + off, n_dp)

    def peer_x(off):
        return z * X + lax.rem(x + off, X)

    def peer_z(off):
        return lax.rem(z + off, Z) * X + x

    barrier = pltpu.get_barrier_semaphore()
    for off in range(1, n_dp):
        pl.semaphore_signal(barrier, 1, device_id={"dp": peer_dp(off)}, device_id_type=MESH)
    for off in range(1, X):
        pl.semaphore_signal(barrier, 1, device_id={"sp": peer_x(off)}, device_id_type=MESH)
    for off in range(1, Z):
        pl.semaphore_signal(barrier, 1, device_id={"sp": peer_z(off)}, device_id_type=MESH)

    @pl.when(sp > 0)
    def _():
        pl.semaphore_signal(barrier, 1, device_id={"sp": sp - 1}, device_id_type=MESH)

    @pl.when(sp < n_sp - 1)
    def _():
        pl.semaphore_signal(barrier, 1, device_id={"sp": sp + 1}, device_id_type=MESH)

    loads[0].wait()
    loads[1].wait()
    w_ref[...] = jnp.concatenate([wv_ref[...], wg_ref[...]], axis=1)
    wall_ref[:, aligned(dp, 128)] = w_ref[aligned(dp, 128), :]
    loads[2].wait()
    vg_ref[32 : 32 + T, :] = dot(x_ref[...], w_ref[...], NN).astype(BF16)

    ends = jnp.where(sp > 0, 1, 0) + jnp.where(sp < n_sp - 1, 1, 0)
    pl.semaphore_wait(barrier, n_dp - 1 + X - 1 + Z - 1 + ends)

    def halo(ref, way, height, base, i):
        if way == 0:
            src, dst, target = base + T - height, base - height, sp + 1
        else:
            src, dst, target = base, base + T, sp - 1
        return pltpu.make_async_remote_copy(
            ref.at[pl.ds(src, height), :],
            ref.at[pl.ds(dst, height), :],
            halo_send.at[i, way],
            halo_recv.at[i, way],
            device_id={"sp": target},
            device_id_type=MESH,
        )

    def vg_halo(way):
        return halo(vg_ref, way, 32, 32, 0)

    def dact_halo(way):
        return halo(dact_ref, way, 16, 16, 1)

    @pl.when(sp < n_sp - 1)
    def _():
        vg_halo(0).start()

    @pl.when(sp > 0)
    def _():
        vg_halo(1).start()

    @pl.when(sp == 0)
    def _():
        vg_ref[0:32, :] = jnp.zeros((32, 2 * CL), BF16)
        dact_ref[0:16, :] = jnp.zeros((16, 2 * CL), F32)

    @pl.when(sp == n_sp - 1)
    def _():
        vg_ref[32 + T : 64 + T, :] = jnp.zeros((32, 2 * CL), BF16)
        dact_ref[16 + T : 32 + T, :] = jnp.zeros((16, 2 * CL), F32)

    def weights(off):
        target = peer_dp(off)
        return pltpu.make_async_remote_copy(
            w_ref.at[aligned(target, 128), :],
            wall_ref.at[:, aligned(dp, 128)],
            wsend.at[off],
            wrecv.at[off],
            device_id={"dp": target},
            device_id_type=MESH,
        )

    far = sorted(range(1, n_dp), key=lambda off: -min(off, n_dp - off))
    first_batch = [o for o in far if min(o, n_dp - o) in (5, 6, 7)]
    second_batch = [o for o in far if min(o, n_dp - o) in (8, 1)]
    third_batch = [o for o in far if min(o, n_dp - o) in (2, 3, 4)]
    for off in first_batch:
        weights(off).start()

    loads[3].wait()
    loads[4].wait()
    d_act = dot(og_ref[...], dw_ref[...], NT)
    dact_ref[16 : 16 + T, :] = jnp.concatenate([d_act, jnp.zeros_like(d_act)], axis=1)

    @pl.when(sp < n_sp - 1)
    def _():
        dact_halo(0).start()

    @pl.when(sp > 0)
    def _():
        dact_halo(1).start()

    E = T + 32
    EP = -(-E // 128) * 128
    mix_ref[E:EP, :] = jnp.zeros((EP - E, CL), F32)
    dact_ref[E:EP, :] = jnp.zeros((EP - E, 2 * CL), F32)

    @pl.when(sp > 0)
    def _():
        vg_halo(0).wait_recv()

    @pl.when(sp < n_sp - 1)
    def _():
        vg_halo(1).wait_recv()

    def gate_block(i):
        rows = aligned(i, 64)
        both = vg_ref[rows, :].astype(F32)
        opening = jax.nn.sigmoid(both[:, CL:])
        open_ref[rows, :] = opening
        glu_ref[rows, :] = both[:, :CL] * opening

    repeat(0, (T + 64) // 64, gate_block)

    def conv_block(i):
        acc = jnp.broadcast_to(cb_ref[...], (32, CL))
        for k in range(KW):
            acc = acc + ck_ref[k : k + 1, :] * glu_ref[pl.ds(i * 32 + k + 1, 32), :]
        mix_ref[aligned(i, 32), :] = acc

    repeat(0, E // 32, conv_block)

    n_blocks = EP // 128
    row8 = lax.broadcasted_iota(jnp.int32, (8, CL), 0)

    def pick(j):
        return jnp.where(row8 == j, 1.0, 0.0).astype(F32)

    def packed(first, second):
        total = None
        for j in range(n_blocks):
            term = exact_dot(pick(j), first(j), NT) + exact_dot(pick(n_blocks + j), second(j), NT)
            total = term if total is None else total + term
        return total

    def rows_of(j):
        return pl.ds(j * 128, 128)

    def stat(phase, off):
        return pltpu.make_async_remote_copy(
            stat_ref.at[phase, dp],
            stat_ref.at[phase, dp],
            ssend.at[phase, off],
            srecv.at[phase, off],
            device_id={"dp": peer_dp(off)},
            device_id_type=MESH,
        )

    def stat_arrived(phase, off):
        src = lax.rem(dp + n_dp - off, n_dp)
        pltpu.make_async_remote_copy(
            stat_ref.at[phase, src],
            stat_ref.at[phase, src],
            ssend.at[phase, off],
            srecv.at[phase, off],
            device_id={"dp": peer_dp(off)},
            device_id_type=MESH,
        ).wait_recv()

    def summed(phase):
        for off in far:
            stat_arrived(phase, off)
        return jnp.sum(stat_ref[phase], axis=0)

    def spread_out(table, j):
        return exact_dot(jnp.transpose(table), pick(j), NN)

    stat_ref[0, dp] = packed(
        lambda j: mix_ref[rows_of(j), :], lambda j: mix_ref[rows_of(j), :] * mix_ref[rows_of(j), :]
    )
    for off in far:
        stat(0, off).start()
    for off in second_batch:
        weights(off).start()

    @pl.when(sp > 0)
    def _():
        dact_halo(0).wait_recv()

    @pl.when(sp < n_sp - 1)
    def _():
        dact_halo(1).wait_recv()

    totals = summed(0) * (1.0 / C)
    mean8 = totals
    power8 = pltpu.roll(totals, 8 - n_blocks, 0)
    inv8 = lax.rsqrt(jnp.maximum(power8 - mean8 * mean8, 0.0) + EPS)
    gain = ng_ref[...]
    shift = ns_ref[...]
    for j in range(n_blocks):
        rows = rows_of(j)
        mean = spread_out(mean8, j)
        inv = spread_out(inv8, j)
        cen = (mix_ref[rows, :] - mean) * inv
        normed = cen * gain + shift
        sig = jax.nn.sigmoid(normed)
        dn = dact_ref[rows, 0:CL] * sig * (1.0 + normed * (1.0 - sig))
        inv_ref[rows, :] = inv
        cen_ref[rows, :] = cen
        act_ref[rows, :] = (normed * sig).astype(BF16)
        dn_ref[rows, :] = dn
        dc_ref[rows, :] = dn * gain
    stat_ref[1, dp] = packed(
        lambda j: dc_ref[rows_of(j), :], lambda j: dc_ref[rows_of(j), :] * cen_ref[rows_of(j), :]
    )
    for off in far:
        stat(1, off).start()
    for off in third_batch:
        weights(off).start()

    def x_copy(src, dst, kind, off):
        return pltpu.make_async_remote_copy(
            src,
            dst,
            xsend.at[kind, off],
            xrecv.at[kind, off],
            device_id={"sp": peer_x(off)},
            device_id_type=MESH,
        )

    def x_part(kind, off):
        src, dst = ((pd_ref, rd_ref), (pv_ref, rv_ref))[kind]
        return x_copy(src.at[lax.rem(x + off, X)], dst.at[off - 1], kind, off)

    wide = D // Z
    fold = PR // 2
    act_own = act_ref[16 : 16 + T, :]

    def down_part(i):
        part = dot(og_ref[:, aligned(i, wide)], act_own, TN).astype(BF16)
        for q in range(X):
            piece = part[q * PR : (q + 1) * PR, :]
            pd_ref[q, i] = jnp.concatenate([piece[:fold], piece[fold:]], axis=1)

    repeat(0, Z, down_part)
    for off in (2, 1, 3):
        x_part(0, off).start()

    totals = summed(1) * (1.0 / C)
    second8 = pltpu.roll(totals, 8 - n_blocks, 0)
    for j in range(n_blocks):
        rows = rows_of(j)
        dm = inv_ref[rows, :] * (
            dc_ref[rows, :] - spread_out(totals, j) - cen_ref[rows, :] * spread_out(second8, j)
        )
        token = sp * T - 16 + j * 128 + lax.broadcasted_iota(jnp.int32, (128, CL), 0)
        dm_ref[rows, :] = jnp.where((token >= 0) & (token < n_sp * T), dm, 0.0)

    def back_block(i):
        acc = jnp.zeros((32, CL), F32)
        for k in range(KW):
            acc = acc + ck_ref[k : k + 1, :] * dm_ref[pl.ds(i * 32 + KW - k, 32), :]
        rows = pl.ds(pl.multiple_of(i * 32 + 32, 32), 32)
        opening = open_ref[rows, :]
        value = vg_ref[rows, 0:CL].astype(F32)
        both = jnp.concatenate([acc * opening, acc * value * opening * (1.0 - opening)], axis=1)
        dvg_ref[aligned(i, 32), :] = both.astype(BF16)

    repeat(0, T // 32, back_block)
    g_ref[:, aligned(dp, 128)] = dvg_ref[...]

    tall = T // CHUNKS
    gather_d = RingGather(
        g_ref, tall, y, c, Y, ring_send.at[0], ring_recv.at[0], pair_send.at[0], pair_recv.at[0]
    )
    gather_o = RingGather(
        out_ref, tall, y, c, Y, ring_send.at[1], ring_recv.at[1], pair_send.at[1], pair_recv.at[1]
    )
    repeat(0, CHUNKS, gather_d.start)

    d_own = dvg_ref[...]

    def value_part(i):
        part = dot(x_ref[:, aligned(i, wide)], d_own, TN).astype(BF16)
        pv_ref[:, i] = part.reshape(X, PR, 2 * CL)

    repeat(0, Z, value_part)
    for off in (2, 1, 3):
        x_part(1, off).start()

    def tap_block(i, taps):
        d = dm_ref[pl.ds(pl.multiple_of(i * 8 + 16, 8), 8), :]
        return tuple(
            t + d * glu_ref[pl.ds(i * 8 + k + 17, 8), :] for k, t in enumerate(taps)
        )

    taps = lax.fori_loop(
        0, T // 8, tap_block, tuple(jnp.zeros((8, CL), F32) for _ in range(KW))
    )
    sums = [jnp.sum(t, axis=0, keepdims=True) for t in taps]
    sums.append(jnp.sum(dm_ref[16 : 16 + T, :], axis=0, keepdims=True))
    sums.append(
        jnp.sum(dn_ref[16 : 16 + T, :] * cen_ref[16 : 16 + T, :], axis=0, keepdims=True)
    )
    sums.append(jnp.sum(dn_ref[16 : 16 + T, :], axis=0, keepdims=True))
    sums.append(jnp.zeros((48 - KW - 3, CL), F32))
    table = jnp.concatenate(sums, axis=0)
    kx_ref[x] = jnp.concatenate([table[:24], table[24:]], axis=1)

    def kx_copy(off):
        return x_copy(kx_ref.at[x], kx_ref.at[x], 2, off)

    for off in (2, 1, 3):
        kx_copy(off).start()

    for h in range(Y // 2):
        gather_d.hop(h)

    for off in far:
        weights(off).wait_recv()

    def product(k):
        gather_d.wait_pairs(k)
        rows = aligned(k, tall)
        out = dot(g_ref[rows, :], wall_ref[...], NT)
        out_ref[rows, aligned(dp, 128)] = out.astype(BF16)
        gather_o.start(k)

    repeat(0, CHUNKS, product)

    def kx_arrived(off):
        src = lax.rem(x + X - off, X)
        return x_copy(kx_ref.at[src], kx_ref.at[src], 2, off)

    for off in (1, 3, 2):
        x_part(0, off).wait_recv()
        x_part(1, off).wait_recv()
        kx_arrived(off).wait_recv()

    def x_sum(i):
        d = pd_ref[x, i].astype(F32)
        v = pv_ref[x, i].astype(F32)
        for slot in range(X - 1):
            d = d + rd_ref[slot, i].astype(F32)
            v = v + rv_ref[slot, i].astype(F32)
        s_ref[i, 0:PR] = v.astype(BF16)
        s_ref[i, PR : PR + fold] = d.astype(BF16)

        @pl.when(i == z)
        def _():
            own_ref[0:PR] = v
            own_ref[PR : PR + fold] = d

    repeat(0, Z, x_sum)
    kz_ref[z] = (kx_ref[0] + kx_ref[1]) + (kx_ref[2] + kx_ref[3])

    def z_copy(src, dst, kind, off):
        return pltpu.make_async_remote_copy(
            src,
            dst,
            zsend.at[kind, off],
            zrecv.at[kind, off],
            device_id={"sp": peer_z(off)},
            device_id_type=MESH,
        )

    def z_part(off):
        return z_copy(s_ref.at[lax.rem(z + off, Z)], rz_ref.at[off - 1], 0, off)

    def kz_copy(off):
        return z_copy(kz_ref.at[z], kz_ref.at[z], 1, off)

    z_far = sorted(range(1, Z), key=lambda off: -min(off, Z - off))
    for off in z_far:
        z_part(off).start()
    for off in z_far:
        kz_copy(off).start()

    for h in range(Y // 2):
        gather_o.hop(h)

    def store(k):
        rows = aligned(k, tall)
        return pltpu.make_async_copy(out_ref.at[rows, :], ig_hbm.at[rows, :], store_sem.at[k])

    def finish(k):
        gather_o.wait_pairs(k)
        store(k).start()

    repeat(0, CHUNKS, finish)

    for off in z_far:
        z_part(off).wait_recv()
    total = own_ref[...]
    for off in range(1, Z):
        total = total + rz_ref[off - 1].astype(F32)
    total = total * ratio
    vg_out[...] = total[0:PR]
    dg_out[...] = total[PR : PR + fold]

    for off in z_far:
        src = lax.rem(z + Z - off, Z)
        z_copy(kz_ref.at[src], kz_ref.at[src], 1, off).wait_recv()
    k_total = kz_ref[0]
    for i in range(1, Z):
        k_total = k_total + kz_ref[i]
    kg_out[...] = k_total * ratio

    @pl.when(sp < n_sp - 1)
    def _():
        vg_halo(0).wait_send()
        dact_halo(0).wait_send()

    @pl.when(sp > 0)
    def _():
        vg_halo(1).wait_send()
        dact_halo(1).wait_send()

    for off in far:
        weights(off).wait_send()
        stat(0, off).wait_send()
        stat(1, off).wait_send()
    for off in range(1, X):
        x_part(0, off).wait_send()
        x_part(1, off).wait_send()
        kx_copy(off).wait_send()
    for off in z_far:
        z_part(off).wait_send()
        kz_copy(off).wait_send()
    gather_d.drain()
    gather_o.drain()
    repeat(0, CHUNKS, lambda k: store(k).wait())


def run(n_sp, n_dp, *args):
    x, og, wv, wg, dw, ck, cb, ng, ns = args
    T, D = x.shape
    CL = wv.shape[1]
    Z, Y = n_sp // X, n_dp // 2
    PR = D // n_sp
    E = T + 32
    EP = -(-E // 128) * 128
    vmem = pl.BlockSpec(memory_space=pltpu.VMEM)
    hbm = pl.BlockSpec(memory_space=pl.ANY)
    dma = pltpu.SemaphoreType.DMA
    half = Y // 2
    V = pltpu.VMEM
    outs = pl.pallas_call(
        functools.partial(kernel, n_sp, n_dp),
        out_shape=(
            jax.ShapeDtypeStruct((T, D), BF16),
            jax.ShapeDtypeStruct((PR, 2 * CL), F32),
            jax.ShapeDtypeStruct((PR // 2, 2 * CL), F32),
            jax.ShapeDtypeStruct((24, 2 * CL), F32),
        ),
        in_specs=[hbm] * 5 + [vmem] * 4,
        out_specs=(hbm, vmem, vmem, vmem),
        scratch_shapes=[
            V((T, D), BF16),
            V((T, D), BF16),
            V((D, CL), BF16),
            V((D, CL), BF16),
            V((CL, D), BF16),
            V((D, 2 * CL), BF16),
            V((128, n_dp * 128), BF16),
            V((T + 64, 2 * CL), BF16),
            V((T + 64, CL), F32),
            V((T + 64, CL), F32),
            V((EP, 2 * CL), F32),
            V((EP, CL), F32),
            V((EP, CL), F32),
            V((EP, CL), F32),
            V((EP, CL), F32),
            V((EP, CL), F32),
            V((EP, CL), BF16),
            V((EP, CL), F32),
            V((T, 2 * CL), BF16),
            V((T, n_dp * 128), BF16),
            V((T, D), BF16),
            V((2, n_dp, 8, 128), F32),
            V((X, Z, PR // 2, 2 * CL), BF16),
            V((X, Z, PR, 2 * CL), BF16),
            V((X - 1, Z, PR // 2, 2 * CL), BF16),
            V((X - 1, Z, PR, 2 * CL), BF16),
            V((Z, PR + PR // 2, 2 * CL), BF16),
            V((PR + PR // 2, 2 * CL), F32),
            V((Z - 1, PR + PR // 2, 2 * CL), BF16),
            V((X, 24, 2 * CL), F32),
            V((Z, 24, 2 * CL), F32),
            dma((5,)),
            dma((2, 2)),
            dma((2, 2)),
            dma((n_dp,)),
            dma((n_dp,)),
            dma((2, n_dp)),
            dma((2, n_dp)),
            dma((2, 2, half, CHUNKS)),
            dma((2, 2, half, CHUNKS)),
            dma((2, Y, CHUNKS)),
            dma((2, Y, CHUNKS)),
            dma((3, X)),
            dma((3, X)),
            dma((2, Z)),
            dma((2, Z)),
            dma((CHUNKS,)),
        ],
        compiler_params=pltpu.CompilerParams(collective_id=0, has_side_effects=True),
    )(x, og, wv, wg, dw, ck, cb[None, :], ng[None, :], ns[None, :])
    ig, vg, dg, kg = outs
    KW = ck.shape[0]
    down = jnp.concatenate([dg[:, :CL], dg[:, CL:]], axis=0).T
    table = jnp.concatenate([kg[:, :CL], kg[:, CL:]], axis=0)
    return (
        ig,
        vg[:, :CL],
        vg[:, CL:],
        down,
        table[:KW],
        table[KW],
        table[KW + 1],
        table[KW + 2],
    )


def solution(mesh):
    n_sp, n_dp = mesh.shape["sp"], mesh.shape["dp"]
    in_specs = (
        P("sp", None),
        P("sp", None),
        P(None, "dp"),
        P(None, "dp"),
        P("dp", None),
        P(None, "dp"),
        P("dp"),
        P("dp"),
        P("dp"),
    )
    out_specs = (
        P("sp", None),
        P("sp", "dp"),
        P("sp", "dp"),
        P("dp", "sp"),
        P(None, "dp"),
        P("dp"),
        P("dp"),
        P("dp"),
    )
    return jax.shard_map(
        functools.partial(run, n_sp, n_dp),
        mesh=mesh,
        in_specs=in_specs,
        out_specs=out_specs,
        check_vma=False,
    )
```
